128 devices in a mesh: sp: 16 (over z, y), tp: 8 (over x, core).
Axes of the slice: x: 4, y: 4, z: 4, core: 2. Of those that a mesh axis runs over, the one named last changes fastest.
Arguments:
- tokens: bfloat16 [12288, 2048], P('sp', 'tp'), may hold values from -6 to 6
- norm_gain: float32 [2048], replicated, may hold values from 0.1 to 1.9
- w_query: bfloat16 [2048, 2048], P(None, 'tp'), may hold values from -4 to 4
- w_key: bfloat16 [2048, 2048], P(None, 'tp'), may hold values from -4 to 4
- w_value: bfloat16 [2048, 2048], P(None, 'tp'), may hold values from -0.125 to 0.125
- w_outer: bfloat16 [2048, 2048], P(None, 'tp'), may hold values from -0.125 to 0.125
- w_inner: bfloat16 [2048, 2048], P(None, 'tp'), may hold values from -0.125 to 0.125
- w_signal: bfloat16 [2048, 2048], P(None, 'tp'), may hold values from -0.125 to 0.125
- conv_taps: bfloat16 [3, 2048], P(None, 'tp'), may hold values from -3.5 to 3.5
- lambdas: float32 [8], P('tp'), may hold values from 0.3 to 0.8
- head_gain: float32 [256], replicated, may hold values from 0.1 to 1.9
- attend_proj: bfloat16 [2048, 2048], P('tp'), may hold values from -0.125 to 0.125
- convolve_proj: bfloat16 [2048, 2048], P('tp'), may hold values from -0.125 to 0.125
Outputs:
- mixed: bfloat16 [12288, 2048], P(('sp', 'tp'))
- row_lse: float32 [12288, 16], P('sp', 'tp')
The draws below stay inside these ranges and needn't reach their ends.
All inputs are finite; a program needn't handle non-finite values.
Results may differ from the reference program's by a relative error of at most 0.015.
Values may be sent and summed in bfloat16 or wider, within the bound.
No kernel may reach another device: no remote copies, remote signals or barrier semaphores. Data moves between devices by JAX's collectives and lax.ppermute only.
A program may use at most 128 MiB of HBM per device.

```python
import math
import jax
import jax.numpy as jnp
from jax import lax

D = 2048
HEADS = 8
HEAD_DIM = 128
CONV = 2048
TOK_DEV = 768
TOKENS = 12288
N_TP = 8


def query_key_pair(key):
    width = 2 * HEADS * HEAD_DIM
    spread = 1.3 / math.sqrt(D)
    key_part = jax.random.normal(jax.random.fold_in(key, 701), (D, width), jnp.float32) * spread
    noise_part = jax.random.normal(jax.random.fold_in(key, 702), (D, width), jnp.float32) * spread
    query_part = noise_part
    return (jnp.clip(query_part, -4.0, 4.0), jnp.clip(key_part, -4.0, 4.0))


def draw_w_query(key, part):
    return query_key_pair(key)[0].astype(jnp.bfloat16)


def draw_w_key(key, part):
    return query_key_pair(key)[1].astype(jnp.bfloat16)


def level_of(rng, dims, cuts, least, top_value):
    def one(position, parts):
        heights = jax.random.uniform(jax.random.fold_in(jax.random.fold_in(rng, 6), position), (parts,), jnp.float32, least / len(cuts), top_value / len(cuts))
        return jnp.repeat(jnp.exp(heights), dims[position] // parts).reshape((-1,) + (1,) * (len(dims) - position - 1))

    loudness = one(*cuts[0])
    for cut in cuts[1:]:
        loudness = loudness * one(*cut)
    return loudness


def bell_draw(rng, shape, scale, limit, pieces=(), kind=jnp.bfloat16):
    level = level_of(rng, shape, pieces, -0.22, 0.18) if pieces else 1.0
    entries = jax.random.normal(rng, shape, jnp.float32) * scale * level
    return jnp.minimum(jnp.maximum(entries, -limit), limit).astype(kind)


def setup_inputs(seed: int = 0) -> dict:
    keys = jax.random.split(jax.random.key(seed), 14)
    return {
        "tokens": bell_draw(keys[0], (TOKENS, D), 1.0, 6.0, ((0, 16), (1, 8))),
        "norm_gain": jnp.clip(1.0 + 0.18 * jax.random.normal(keys[1], (D,), jnp.float32), 0.1, 1.9),
        "w_query": draw_w_query(jax.random.fold_in(keys[13], 71), 0),
        "w_key": draw_w_key(jax.random.fold_in(keys[13], 71), 0),
        "w_value": bell_draw(keys[4], (D, 2 * HEADS * HEAD_DIM), D ** -0.5, 0.125, ((1, 8),)),
        "w_outer": bell_draw(keys[5], (D, CONV), D ** -0.5, 0.125, ((1, 8),)),
        "w_inner": bell_draw(keys[6], (D, CONV), D ** -0.5, 0.125, ((1, 8),)),
        "w_signal": bell_draw(keys[7], (D, CONV), D ** -0.5, 0.125, ((1, 8),)),
        "conv_taps": bell_draw(keys[8], (3, CONV), 3 ** -0.5, 3.5, ((1, 8),)),
        "lambdas": jnp.clip(0.3 + 0.5 * jax.random.uniform(keys[9], (HEADS,), jnp.float32) ** level_of(keys[9], (HEADS,), ((0, 8),), -0.2, 0.2), 0.3, 0.8),
        "head_gain": jnp.clip(1.0 + 0.18 * jax.random.normal(keys[10], (2 * HEAD_DIM,), jnp.float32), 0.1, 1.9),
        "attend_proj": bell_draw(keys[11], (2 * HEADS * HEAD_DIM, D), (2 * HEADS * HEAD_DIM) ** -0.5, 0.125, ((0, 8),)),
        "convolve_proj": bell_draw(keys[12], (CONV, D), CONV ** -0.5, 0.125, ((0, 8),)),
    }


ROPE_BASE = 500000.0
NORM_EPS = 1e-05
HEAD_KEEP = 0.8
MASKED = -1e+30

def rotate(values_in, positions):
    half_width = values_in.shape[-1] // 2
    inverse = ROPE_BASE ** (-jnp.arange(half_width, dtype=jnp.float32) * 2.0 / values_in.shape[-1])
    angles = positions.astype(jnp.float32)[:, None] * inverse[None, :]
    cosine = jnp.cos(angles)[:, None, :]
    sine_part = jnp.sin(angles)[:, None, :]
    first_half = values_in[..., :half_width]
    second_half = values_in[..., half_width:]
    return jnp.concatenate([first_half * cosine - second_half * sine_part, second_half * cosine + first_half * sine_part], axis=-1)

def reference(tokens, norm_gain, w_query, w_key, w_value, w_outer, w_inner, w_signal, conv_taps, lambdas, head_gain, attend_proj, convolve_proj):
    row_count = tokens.shape[0]
    widened = tokens.astype(jnp.float32)
    scaled = (widened * norm_gain[None, :]).astype(jnp.bfloat16)
    inv_rms = lax.rsqrt(lax.optimization_barrier(jnp.mean(widened * widened, axis=1, keepdims=True)) + NORM_EPS)

    def project(weight):
        return inv_rms * jnp.dot(scaled, weight, preferred_element_type=jnp.float32)
    positions = jnp.arange(row_count, dtype=jnp.int32)
    queries = rotate(project(w_query).reshape(row_count, 2 * HEADS, HEAD_DIM), positions).astype(jnp.bfloat16)
    key_rows = rotate(project(w_key).reshape(row_count, 2 * HEADS, HEAD_DIM), positions).astype(jnp.bfloat16)
    value_rows = project(w_value).astype(jnp.bfloat16).reshape(row_count, HEADS, 2 * HEAD_DIM)
    block_count = row_count // TOK_DEV
    key_places = jnp.arange(row_count, dtype=jnp.int32)
    attended_heads = []
    lse_heads = []
    for head_index in range(HEADS):
        head_query = queries[:, 2 * head_index:2 * head_index + 2, :].astype(jnp.float32)
        head_key = key_rows[:, 2 * head_index:2 * head_index + 2, :].astype(jnp.float32)
        head_value = value_rows[:, head_index, :].astype(jnp.float32)
        head_lambda = lambdas[head_index]

        def one_block(block_index):
            first_row = block_index * TOK_DEV
            query_block = lax.dynamic_slice_in_dim(head_query, first_row, TOK_DEV, 0)
            scores = jnp.einsum('qjd,kjd->jqk', query_block, head_key) * HEAD_DIM ** (-0.5)
            query_places = first_row + jnp.arange(TOK_DEV, dtype=jnp.int32)
            allowed = key_places[None, :] <= query_places[:, None]
            scores = jnp.where(allowed[None], scores, MASKED)
            running_max = lax.optimization_barrier(jnp.max(scores, axis=2, keepdims=True))
            lifted = jnp.exp(scores - running_max)
            weight_sum = lax.optimization_barrier(jnp.sum(lifted, axis=2, keepdims=True))
            weights = lax.optimization_barrier((lifted / weight_sum).astype(jnp.bfloat16))
            mixed_pair = jnp.einsum('jqk,ke->jqe', weights.astype(jnp.float32), head_value)
            difference = mixed_pair[0] - head_lambda * mixed_pair[1]
            scale_back = lax.rsqrt(lax.optimization_barrier(jnp.mean(difference * difference, axis=1, keepdims=True)) + NORM_EPS)
            normed = (difference * scale_back * head_gain[None, :] * HEAD_KEEP).astype(jnp.bfloat16)
            log_sum = jnp.transpose((running_max + jnp.log(weight_sum))[:, :, 0], (1, 0))
            return (normed, log_sum)
        normed_blocks, lse_blocks = lax.map(one_block, jnp.arange(block_count, dtype=jnp.int32))
        attended_heads.append(normed_blocks.reshape(row_count, 2 * HEAD_DIM))
        lse_heads.append(lse_blocks.reshape(row_count, 2))
    attended = jnp.concatenate(attended_heads, axis=1)
    row_lse = jnp.concatenate(lse_heads, axis=1)
    product = project(w_inner) * project(w_signal)
    padded = jnp.concatenate([jnp.zeros((2, CONV), jnp.float32), product], axis=0)
    tap_values = conv_taps.astype(jnp.float32)
    smoothed = tap_values[0] * padded[:-2] + tap_values[1] * padded[1:-1] + tap_values[2] * padded[2:]
    convolved = (project(w_outer) * smoothed).astype(jnp.bfloat16)
    head_columns = HEADS // N_TP * 2 * HEAD_DIM
    channel_columns = CONV // N_TP
    summed = jnp.zeros((row_count, D), jnp.float32)
    for group_index in range(N_TP):
        head_lo = group_index * head_columns
        chan_lo = group_index * channel_columns
        partial_value = jnp.dot(attended[:, head_lo:head_lo + head_columns], attend_proj[head_lo:head_lo + head_columns], preferred_element_type=jnp.float32)
        partial_value = partial_value + jnp.dot(convolved[:, chan_lo:chan_lo + channel_columns], convolve_proj[chan_lo:chan_lo + channel_columns], preferred_element_type=jnp.float32)
        rounded = lax.optimization_barrier(partial_value.astype(jnp.bfloat16))
        summed = summed + rounded.astype(jnp.float32)
    return (summed.astype(jnp.bfloat16), row_lse)
```

```python
import functools
import math
import jax
import jax.numpy as jnp
from jax import lax
from jax.experimental import pallas as pl
from jax.experimental.pallas import tpu as pltpu
from jax.sharding import PartitionSpec as P

ROPE_BASE = 500000.0
NORM_EPS = 1e-05
HEAD_KEEP = 0.8
MASKED = -1e30
LOG2E = math.log2(math.e)
LN2 = math.log(2.0)
TQ = 256
SIDE = 4
ROUND_ROWS = 16
AXES = ("sp", "tp")
F32 = jnp.float32
BF16 = jnp.bfloat16


def place_shift(sp, core, steps, along_keys):
    z, y = sp // SIDE, sp % SIDE
    if (core == 0) == along_keys:
        return z * SIDE + (y + steps) % SIDE
    return ((z + steps) % SIDE) * SIDE + y


def side_perm(steps, along_keys):
    return [
        (sp * 8 + tp, place_shift(sp, tp % 2, steps, along_keys) * 8 + tp)
        for sp in range(16)
        for tp in range(8)
    ]


def send_side(value, steps, along_keys):
    return lax.ppermute(value, AXES, side_perm(steps, along_keys))


def neighbour_ids(along_keys):
    sp = lax.axis_index("sp")
    core = lax.axis_index("tp") % 2
    z, y = sp // SIDE, sp % SIDE
    own = []
    for steps in (0, -1, 1, 2):
        by_y = z * SIDE + (y + steps) % SIDE
        by_z = ((z + steps) % SIDE) * SIDE + y
        zero = by_y if along_keys else by_z
        one = by_z if along_keys else by_y
        own.append(jnp.where(core == 0, zero, one))
    return jnp.stack(own).astype(jnp.int32)


def gather_side(value, along_keys):
    half = value.shape[0] // 2
    below = send_side(value, 1, along_keys)
    above = send_side(value, -1, along_keys)
    far_top = send_side(below[:half], 1, along_keys)
    far_bottom = send_side(above[half:], -1, along_keys)
    return value, below, above, far_top, far_bottom


def lanes(value, count):
    return jnp.concatenate([value] * count, axis=1)


def absorb_pair(q_ref, qi, kv_ref, ki, m_ref, l_ref, acc_ref, diagonal):
    rows_all = q_ref.shape[1]
    tiles = rows_all // TQ
    chains = [(tile, j) for tile in range(tiles) for j in range(2)]

    def keys_of(tile):
        return (tile + 1) * TQ if diagonal else rows_all

    def raw_scores(tile, j):
        return lax.dot_general(
            q_ref[qi, tile * TQ : (tile + 1) * TQ, j * 128 : (j + 1) * 128],
            kv_ref[ki, : keys_of(tile), j * 128 : (j + 1) * 128],
            (((1,), (1,)), ((), ())),
            preferred_element_type=F32,
        )

    following = raw_scores(*chains[0])
    for step, (tile, j) in enumerate(chains):
        scores = following
        if step + 1 < len(chains):
            following = raw_scores(*chains[step + 1])
        rows = slice(tile * TQ, (tile + 1) * TQ)
        narrow = slice(j * 128, (j + 1) * 128)
        wide = slice(j * 256, (j + 1) * 256)
        keys = keys_of(tile)
        if diagonal:
            row_place = lax.broadcasted_iota(jnp.int32, (TQ, keys), 0) + tile * TQ
            key_place = lax.broadcasted_iota(jnp.int32, (TQ, keys), 1)
            scores = jnp.where(key_place <= row_place, scores, MASKED)
        before = m_ref[rows, narrow]
        raised = jnp.maximum(before, jnp.max(scores, axis=1, keepdims=True))
        factor = jnp.exp2(before - raised)
        lifted = jnp.exp2(scores - lanes(raised, keys // 128))
        total = factor * l_ref[rows, narrow]
        for part in range(keys // 128):
            total = total + lifted[:, part * 128 : (part + 1) * 128]
        l_ref[rows, narrow] = total
        m_ref[rows, narrow] = raised
        product = jnp.dot(
            lifted.astype(BF16), kv_ref[ki, :keys, 256:512], preferred_element_type=F32
        )
        acc_ref[rows, wide] = acc_ref[rows, wide] * lanes(factor, 2) + product


def settle(m_ref, l_ref, acc_ref, rows, j):
    total = jnp.sum(l_ref[rows, j * 128 : (j + 1) * 128], axis=1, keepdims=True)
    total = jnp.where(total == 0.0, 1.0, total)
    mean = acc_ref[rows, j * 256 : (j + 1) * 256] / total
    lse = m_ref[rows, j * 128 : (j + 1) * 128] + jnp.log(total) * LOG2E
    return mean, lse


def pack_half(means, lses, out_ref, lead, line_ref):
    half = means[0].shape[0]
    line_ref[...] = jnp.zeros_like(line_ref)
    for j in range(2):
        out_ref[lead + (slice(0, half), slice(j * 256, (j + 1) * 256))] = means[j].astype(BF16)
        line = jnp.transpose(lses[j])[0:1, :]
        for piece in range(3):
            part = line.astype(BF16).astype(F32)
            line_ref[3 * j + piece : 3 * j + piece + 1, :half] = part
            line = line - part
    out_ref[lead + (slice(half, half + ROUND_ROWS), slice(None))] = line_ref[...].astype(BF16)


def unpack_half(ref, half):
    tail = ref[half : half + ROUND_ROWS, :].astype(F32)
    means, lses = [], []
    for j in range(2):
        means.append(ref[:half, j * 256 : (j + 1) * 256].astype(F32))
        line = tail[3 * j : 3 * j + 1] + tail[3 * j + 1 : 3 * j + 2] + tail[3 * j + 2 : 3 * j + 3]
        lses.append(jnp.transpose(jnp.broadcast_to(line[:, :half], (128, half))))
    return means, lses


def merge(first, second):
    (mean_a, lse_a), (mean_b, lse_b) = first, second
    top = jnp.maximum(lse_a, lse_b)
    weight_a = jnp.exp2(lse_a - top)
    weight_b = jnp.exp2(lse_b - top)
    total = weight_a + weight_b
    mean = mean_a * lanes(weight_a / total, 2) + mean_b * lanes(weight_b / total, 2)
    return mean, top + jnp.log(total) * LOG2E


def load_start(sources, targets, sems):
    copies = []
    for source, target, sem in zip(sources, targets, sems):
        copy = pltpu.make_async_copy(source, target, sem)
        copy.start()
        copies.append(copy)
    return copies


def reset(m_ref, l_ref, acc_ref):
    m_ref[...] = jnp.full_like(m_ref, MASKED)
    l_ref[...] = jnp.zeros_like(l_ref)
    acc_ref[...] = jnp.zeros_like(acc_ref)


def own_kernel(ids, q_hbm, kv0, kv1, kv2, mean_ref, lse_ref, q_s, kv_s, m_s, l_s, acc_s, sems):
    copies = load_start(
        (kv0, q_hbm, kv1, kv2),
        (kv_s.at[0], q_s.at[0], kv_s.at[1], kv_s.at[2]),
        [sems.at[i] for i in range(4)],
    )
    reset(m_s, l_s, acc_s)
    copies[0].wait()
    copies[1].wait()
    absorb_pair(q_s, 0, kv_s, 0, m_s, l_s, acc_s, True)
    copies[2].wait()
    copies[3].wait()

    def step(ki, none):
        @pl.when(ids[1, ki] < ids[0, 0])
        def _():
            absorb_pair(q_s, 0, kv_s, ki, m_s, l_s, acc_s, False)

        return none

    lax.fori_loop(1, 3, step, 0)
    for j in range(2):
        mean, lse = settle(m_s, l_s, acc_s, slice(None), j)
        mean_ref[:, j * 256 : (j + 1) * 256] = mean
        lse_ref[:, j * 128 : (j + 1) * 128] = lse


def far_kernel(first_q, q_count, ids, *refs):
    q_refs = refs[: q_count if first_q == 1 else 2]
    kv_refs = refs[len(q_refs) : len(q_refs) + 5]
    out_ref = refs[len(q_refs) + 5]
    q_s, kv_s, m_s, l_s, acc_s, line_s, sems = refs[len(q_refs) + 6 :]
    rows = q_s.shape[1]
    half = rows // 2
    if first_q == 1:
        q_targets = [q_s.at[i] for i in range(q_count)]
    else:
        q_targets = [q_s.at[0, :half], q_s.at[0, half:]]
    kv_targets = [kv_s.at[0], kv_s.at[1], kv_s.at[2], kv_s.at[3, :half], kv_s.at[3, half:]]
    all_sources = list(q_refs) + list(kv_refs)
    copies = load_start(
        all_sources, q_targets + kv_targets, [sems.at[i] for i in range(len(all_sources))]
    )
    for copy in copies:
        copy.wait()

    def one_query(qi, _):
        reset(m_s, l_s, acc_s)
        q_id = ids[0, first_q + qi]

        def step(ki, none):
            @pl.when(ids[1, ki] < q_id)
            def _():
                absorb_pair(q_s, qi, kv_s, ki, m_s, l_s, acc_s, False)

            return none

        lax.fori_loop(0, 4, step, 0)
        for part in range(2):
            span = slice(part * half, (part + 1) * half)
            pairs = [settle(m_s, l_s, acc_s, span, j) for j in range(2)]
            pack_half(
                [p[0] for p in pairs], [p[1] for p in pairs], out_ref, (qi, part), line_s
            )
        return _

    lax.fori_loop(0, q_count, one_query, 0)


def merge_kernel(a_ref, b_ref, out_ref, line_s):
    half = a_ref.shape[0] - ROUND_ROWS
    means_a, lses_a = unpack_half(a_ref, half)
    means_b, lses_b = unpack_half(b_ref, half)
    merged = [merge((means_a[j], lses_a[j]), (means_b[j], lses_b[j])) for j in range(2)]
    pack_half([m[0] for m in merged], [m[1] for m in merged], out_ref, (), line_s)


def final_kernel(
    ids, lam_ref, q_hbm, kv_top, kv_bottom, mean_in, lse_in, gain_ref, r0, r1, r2, r3,
    att_ref, lse_ref, q_s, kv_s, m_s, l_s, acc_s, sems,
):
    rows = q_s.shape[1]
    half = rows // 2
    copies = load_start(
        (q_hbm, kv_top, kv_bottom),
        (q_s.at[0], kv_s.at[0, :half], kv_s.at[0, half:]),
        [sems.at[i] for i in range(3)],
    )
    reset(m_s, l_s, acc_s)
    for copy in copies:
        copy.wait()

    @pl.when(ids[1, 3] < ids[0, 0])
    def _():
        absorb_pair(q_s, 0, kv_s, 0, m_s, l_s, acc_s, False)

    for part in range(2):
        span = slice(part * half, (part + 1) * half)
        first_means, first_lses = unpack_half((r0, r1)[part], half)
        second_means, second_lses = unpack_half((r2, r3)[part], half)
        result = []
        for j in range(2):
            state = settle(m_s, l_s, acc_s, span, j)
            state = merge(
                state,
                (mean_in[span, j * 256 : (j + 1) * 256], lse_in[span, j * 128 : (j + 1) * 128]),
            )
            state = merge(state, (first_means[j], first_lses[j]))
            state = merge(state, (second_means[j], second_lses[j]))
            result.append(state[0])
            lse_ref[span, j : j + 1] = state[1][:, 0:1] * LN2
        difference = result[0] - lam_ref[0] * result[1]
        mean_square = jnp.mean(difference * difference, axis=1, keepdims=True)
        scaled = difference * lax.rsqrt(mean_square + NORM_EPS) * gain_ref[...] * HEAD_KEEP
        att_ref[span, :] = scaled.astype(BF16)


ANY = pl.BlockSpec(memory_space=pl.ANY)
VM = pl.BlockSpec(memory_space=pltpu.VMEM)
SM = pl.BlockSpec(memory_space=pltpu.SMEM)


def attention_scratch(rows, q_count, kv_count, copies, line):
    shapes = [
        pltpu.VMEM((q_count, rows, 256), BF16),
        pltpu.VMEM((kv_count, rows, 512), BF16),
        pltpu.VMEM((rows, 256), F32),
        pltpu.VMEM((rows, 256), F32),
        pltpu.VMEM((rows, 512), F32),
    ]
    if line:
        shapes.append(pltpu.VMEM((ROUND_ROWS, 512), F32))
    return shapes + [pltpu.SemaphoreType.DMA((copies,))]


def cost(pairs, rows):
    return pl.CostEstimate(
        flops=int(pairs * rows * rows * 128 * 2 * 6),
        transcendentals=int(pairs * rows * rows * 2),
        bytes_accessed=8 * 2**20,
    )


def attend(queries, key_values, lam, head_gain):
    rows = queries.shape[0]
    half = rows // 2
    ids = jnp.stack([neighbour_ids(False), neighbour_ids(True)])
    q0, q1, q2, q3t, q3b = gather_side(queries, False)
    k0, k1, k2, k3t, k3b = gather_side(key_values, True)
    params = pltpu.CompilerParams(vmem_limit_bytes=56 * 2**20)
    mean_own, lse_own = pl.pallas_call(
        own_kernel,
        name="own",
        out_shape=(
            jax.ShapeDtypeStruct((rows, 512), F32),
            jax.ShapeDtypeStruct((rows, 256), F32),
        ),
        in_specs=[SM, ANY, ANY, ANY, ANY],
        out_specs=(VM, VM),
        scratch_shapes=attention_scratch(rows, 1, 3, 4, False),
        compiler_params=params,
        cost_estimate=cost(2.5, rows),
    )(ids, q0, k0, k1, k2)
    far = pl.pallas_call(
        functools.partial(far_kernel, 3, 1),
        name="far",
        out_shape=jax.ShapeDtypeStruct((1, 2, half + ROUND_ROWS, 512), BF16),
        in_specs=[SM] + [ANY] * 7,
        out_specs=VM,
        scratch_shapes=attention_scratch(rows, 1, 4, 7, True),
        compiler_params=params,
        cost_estimate=cost(4, rows),
    )(ids, q3t, q3b, k0, k1, k2, k3t, k3b)
    from_below = send_side(far[0, 0], 1, False)
    from_above = send_side(far[0, 1], -1, False)
    near = pl.pallas_call(
        functools.partial(far_kernel, 1, 2),
        name="near",
        out_shape=jax.ShapeDtypeStruct((2, 2, half + ROUND_ROWS, 512), BF16),
        in_specs=[SM] + [ANY] * 7,
        out_specs=VM,
        scratch_shapes=attention_scratch(rows, 2, 4, 7, True),
        compiler_params=params,
        cost_estimate=cost(8, rows),
    )(ids, q1, q2, k0, k1, k2, k3t, k3b)

    def merged(first, second):
        return pl.pallas_call(
            merge_kernel,
            name="merge",
            out_shape=jax.ShapeDtypeStruct((half + ROUND_ROWS, 512), BF16),
            in_specs=[VM, VM],
            out_specs=VM,
            scratch_shapes=[pltpu.VMEM((ROUND_ROWS, 512), F32)],
        )(first, second)

    above_top = send_side(near[0, 0], -1, False)
    below_bottom = send_side(near[1, 1], 1, False)
    above_bottom = send_side(merged(near[0, 1], from_above), -1, False)
    below_top = send_side(merged(near[1, 0], from_below), 1, False)
    return pl.pallas_call(
        final_kernel,
        name="final",
        out_shape=(
            jax.ShapeDtypeStruct((rows, 256), BF16),
            jax.ShapeDtypeStruct((rows, 2), F32),
        ),
        in_specs=[SM, SM, ANY, ANY, ANY] + [VM] * 7,
        out_specs=(VM, VM),
        scratch_shapes=attention_scratch(rows, 1, 1, 3, False),
        compiler_params=params,
        cost_estimate=cost(1, rows),
    )(
        ids, lam, q0, k3t, k3b, mean_own, lse_own, head_gain.reshape(1, 256),
        above_top, above_bottom, below_top, below_bottom,
    )


def rotate(values_in, positions):
    half_width = values_in.shape[-1] // 2
    inverse = ROPE_BASE ** (-jnp.arange(half_width, dtype=F32) * 2.0 / values_in.shape[-1])
    angles = positions.astype(F32)[:, None] * inverse[None, :]
    cosine = jnp.cos(angles)[:, None, :]
    sine_part = jnp.sin(angles)[:, None, :]
    first_half = values_in[..., :half_width]
    second_half = values_in[..., half_width:]
    return jnp.concatenate(
        [
            first_half * cosine - second_half * sine_part,
            second_half * cosine + first_half * sine_part,
        ],
        axis=-1,
    )


def per_device(
    tokens, norm_gain, w_query, w_key, w_value, w_outer, w_inner, w_signal, conv_taps,
    lambdas, head_gain, attend_proj, convolve_proj,
):
    row_count = tokens.shape[0]
    model_width = norm_gain.shape[0]
    widened = lax.all_gather(tokens, "tp", axis=1, tiled=True).astype(F32)
    scaled = (widened * norm_gain[None, :]).astype(BF16)
    squares = jnp.sum(widened * widened, axis=1)
    inv_rms = lax.rsqrt(squares / model_width + NORM_EPS)[:, None]

    def project(weight):
        return inv_rms * jnp.dot(scaled, weight, preferred_element_type=F32)

    positions = lax.axis_index("sp") * row_count + jnp.arange(row_count, dtype=jnp.int32)
    score_scale = 128 ** (-0.5) * LOG2E
    queries = rotate(project(w_query).reshape(row_count, 2, 128), positions)
    queries = (queries * score_scale).astype(BF16).reshape(row_count, 256)
    key_rows = rotate(project(w_key).reshape(row_count, 2, 128), positions)
    key_rows = key_rows.astype(BF16).reshape(row_count, 256)
    key_values = jnp.concatenate([key_rows, project(w_value).astype(BF16)], axis=1)
    attended, row_lse = attend(queries, key_values, lambdas, head_gain)

    product = project(w_inner) * project(w_signal)
    border = lax.ppermute(product[row_count - 2 :], "sp", [(i, i + 1) for i in range(15)])
    padded = jnp.concatenate([border, product], axis=0)
    tap_values = conv_taps.astype(F32)
    smoothed = (
        tap_values[0] * padded[:-2] + tap_values[1] * padded[1:-1] + tap_values[2] * padded[2:]
    )
    convolved = (project(w_outer) * smoothed).astype(BF16)
    mixed = lax.psum_scatter(
        (
            jnp.dot(attended, attend_proj, preferred_element_type=F32)
            + jnp.dot(convolved, convolve_proj, preferred_element_type=F32)
        ).astype(BF16),
        "tp",
        scatter_dimension=0,
        tiled=True,
    )
    return (mixed, row_lse)


def solution(mesh):
    return jax.shard_map(
        per_device,
        mesh=mesh,
        in_specs=(P("sp", "tp"), P()) + (P(None, "tp"),) * 7 + (P("tp"), P())
        + (P("tp", None),) * 2,
        out_specs=(P(("sp", "tp"), None), P("sp", "tp")),
        check_vma=False,
    )
```
